32 devices in a mesh: sp: 16 (over z, y, x), tp: 2 (over core).
Axes of the slice: x: 2, y: 2, z: 4, core: 2. Of those that a mesh axis runs over, the one named last changes fastest.
Arguments:
- queries: bfloat16 [4096, 1024], P('sp', 'tp'), may hold values from -6 to 6
- keys: bfloat16 [4096, 512], P('sp', 'tp'), may hold values from -6 to 6
- values: bfloat16 [4096, 512], P('sp', 'tp'), may hold values from -6 to 6
- q_gain: float32 [64], replicated, may hold values from 1.6 to 4.5
- key_norm_gain: float32 [64], replicated, may hold values from 1.6 to 4.5
- out_weight: bfloat16 [1024, 2048], P('tp'), may hold values from -0.1875 to 0.1875
- residual: bfloat16 [4096, 2048], P('sp'), may hold values from -6 to 6
- ln1_gain: float32 [2048], replicated, may hold values from 0.1 to 1.9
- ln1_bias: float32 [2048], replicated, may hold values from -3 to 3
- up_weight: bfloat16 [2048, 8192], P('sp', 'tp'), may hold values from -0.125 to 0.125
- down_weight: bfloat16 [8192, 2048], P('tp', 'sp'), may hold values from -0.0625 to 0.0625
- ln2_gain: float32 [2048], replicated, may hold values from 0.1 to 1.9
- ln2_bias: float32 [2048], replicated, may hold values from -3 to 3
Outputs:
- encoded: bfloat16 [4096, 2048], P('sp', 'tp')
The draws below stay inside these ranges and needn't reach their ends.
All inputs are finite; a program needn't handle non-finite values.
Results may differ from the reference program's by a relative error of at most 0.014.
Values may be sent and summed in bfloat16 or wider, within the bound.
No kernel may reach another device: no remote copies, remote signals or barrier semaphores. Data moves between devices by JAX's collectives and lax.ppermute only.
A program may use at most 128 MiB of HBM per device.

```python
import math
import jax
import jax.numpy as jnp
from jax import lax

D = 2048
FF = 8192
QUERY_HEADS = 16
KEY_VALUE_HEADS = 8
HEAD_SIZE = 64
GRID_W = 64
SEQUENCE_TOKENS = 4096
N_TP = 2


def random_base_keys(key):
    return jnp.clip(jax.random.normal(jax.random.fold_in(key, 11), (SEQUENCE_TOKENS, KEY_VALUE_HEADS * HEAD_SIZE), jnp.float32), -6.0, 6.0)


def draw_keys(key, part):
    return random_base_keys(key).astype(jnp.bfloat16)


def draw_queries(key, part):
    drawn_q = jnp.clip(jax.random.normal(jax.random.fold_in(key, 12), (SEQUENCE_TOKENS, QUERY_HEADS * HEAD_SIZE), jnp.float32), -6.0, 6.0)
    return drawn_q.astype(jnp.bfloat16)


def draw_q_gain(key, part):
    return jax.random.uniform(jax.random.fold_in(key, 21), (HEAD_SIZE,), jnp.float32, 1.6, 2.4)


def draw_key_norm_gain(key, part):
    return jax.random.uniform(jax.random.fold_in(key, 22), (HEAD_SIZE,), jnp.float32, 1.6, 2.4)


def block_levels(rng, extent, cuts, least, high):
    level, own = 1.0, jax.random.fold_in(rng, 6)
    for dim, blocks in cuts:
        heights = jnp.exp(jax.random.uniform(jax.random.fold_in(own, dim), (blocks,), jnp.float32, least / len(cuts), high / len(cuts)))
        level = level * jnp.repeat(heights, extent[dim] // blocks).reshape([-1 if axis == dim else 1 for axis in range(len(extent))])
    return level


def gaussian(key, extent, scale, limit, shards=(), kind=jnp.bfloat16):
    values = jax.random.normal(key, extent, jnp.float32) * scale
    if len(shards) > 0:
        values = block_levels(key, extent, shards, -0.22, 0.18) * values
    return jnp.clip(values, min=-limit, max=limit).astype(kind)


def setup_inputs(seed: int = 0) -> dict:
    key_list = jax.random.split(jax.random.key(seed), 14)
    return {
        "queries": draw_queries(jax.random.fold_in(key_list[13], 71), 0),
        "keys": draw_keys(jax.random.fold_in(key_list[13], 71), 0),
        "values": gaussian(key_list[2], (SEQUENCE_TOKENS, KEY_VALUE_HEADS * HEAD_SIZE), 1.0, 6.0, ((0, 16), (1, 2))),
        "q_gain": draw_q_gain(jax.random.fold_in(key_list[13], 71), 0),
        "key_norm_gain": draw_key_norm_gain(jax.random.fold_in(key_list[13], 71), 0),
        "out_weight": gaussian(key_list[5], (QUERY_HEADS * HEAD_SIZE, D), (QUERY_HEADS * HEAD_SIZE) ** -0.5, 0.1875, ((0, 2),)),
        "residual": gaussian(key_list[6], (SEQUENCE_TOKENS, D), 1.0, 6.0, ((0, 16),)),
        "ln1_gain": jnp.clip(1.0 + 0.18 * jax.random.normal(key_list[7], (D,), jnp.float32), 0.1, 1.9),
        "ln1_bias": gaussian(key_list[8], (D,), 0.3, 3.0, (), jnp.float32),
        "up_weight": gaussian(key_list[9], (D, FF), D ** -0.5, 0.125, ((0, 16), (1, 2))),
        "down_weight": gaussian(key_list[10], (FF, D), FF ** -0.5, 0.0625, ((0, 2), (1, 16))),
        "ln2_gain": jnp.clip(1.0 + 0.18 * jax.random.normal(key_list[11], (D,), jnp.float32), 0.1, 1.9),
        "ln2_bias": gaussian(key_list[12], (D,), 0.3, 3.0, (), jnp.float32),
    }


ALPHA = 8.0 ** 0.25
ROTARY_BASE = 10000.0
RMS_EPSILON = 1e-06
NORM_EPSILON = 1e-05

def rotate_grid(heads_in, grid_places):
    half_dim = heads_in.shape[-1] // 2
    quarter = half_dim // 2
    inverse = ROTARY_BASE ** (-jnp.arange(quarter, dtype=jnp.float32) / quarter)

    def spin(segment, coords):
        angles = coords.astype(jnp.float32)[:, None] * inverse[None, :]
        cos_val = jnp.cos(angles)[:, None, :]
        sin_val = jnp.sin(angles)[:, None, :]
        lead_half = segment[..., :quarter]
        tail_half = segment[..., quarter:]
        return jnp.concatenate([lead_half * cos_val - tail_half * sin_val, tail_half * cos_val + lead_half * sin_val], -1)
    return jnp.concatenate([spin(heads_in[..., :half_dim], grid_places // GRID_W), spin(heads_in[..., half_dim:], grid_places % GRID_W)], -1)

def prepare_inputs(heads_in, gain_vec, grid_places, factor):
    values32 = heads_in.astype(jnp.float32)
    normed = values32 * lax.rsqrt(lax.optimization_barrier(jnp.mean(values32 * values32, -1, keepdims=True)) + RMS_EPSILON) * gain_vec
    return (rotate_grid(normed, grid_places) * factor).astype(jnp.bfloat16)

def layer_norm(pre_norm, gain_vec, bias_vec):
    row_mean = lax.optimization_barrier(jnp.mean(pre_norm, -1, keepdims=True))
    centred = pre_norm - row_mean
    spread = lax.optimization_barrier(jnp.mean(centred * centred, -1, keepdims=True))
    return centred * lax.rsqrt(spread + NORM_EPSILON) * gain_vec + bias_vec

def sum_partials(left_side, right_side):
    group_width = left_side.shape[1] // N_TP
    totals = jnp.zeros((left_side.shape[0], right_side.shape[1]), jnp.float32)
    for member in range(N_TP):
        partial_value = jnp.dot(left_side[:, member * group_width:(member + 1) * group_width], right_side[member * group_width:(member + 1) * group_width], preferred_element_type=jnp.float32)
        totals = totals + lax.optimization_barrier(partial_value.astype(jnp.bfloat16)).astype(jnp.float32)
    return totals

def reference(queries, keys, values, q_gain, key_norm_gain, out_weight, residual, ln1_gain, ln1_bias, up_weight, down_weight, ln2_gain, ln2_bias):
    sequence_length = queries.shape[0]
    grid_places = jnp.arange(sequence_length, dtype=jnp.int32)
    group_count_size = QUERY_HEADS // KEY_VALUE_HEADS
    single_query_block = math.gcd(sequence_length, 128)
    query_head_rows = prepare_inputs(queries.reshape(sequence_length, QUERY_HEADS, HEAD_SIZE), q_gain, grid_places, HEAD_SIZE ** (-0.5))
    key_head_rows = prepare_inputs(keys.reshape(sequence_length, KEY_VALUE_HEADS, HEAD_SIZE), key_norm_gain, grid_places, 1.0).astype(jnp.float32)
    value_head_rows = values.reshape(sequence_length, KEY_VALUE_HEADS, HEAD_SIZE).astype(jnp.float32)
    query_block_list = query_head_rows.reshape(sequence_length // single_query_block, single_query_block, KEY_VALUE_HEADS, group_count_size, HEAD_SIZE)

    def attend(q_block):
        scores = jnp.einsum('qhgd,khd->hgqk', q_block.astype(jnp.float32), key_head_rows)
        maxima = lax.optimization_barrier(jnp.max(scores, -1, keepdims=True))
        weights = jnp.exp(scores - maxima)
        totals = lax.optimization_barrier(jnp.sum(weights, -1))
        rounded = lax.optimization_barrier(weights.astype(jnp.bfloat16)).astype(jnp.float32)
        summed = jnp.einsum('hgqk,khd->qhgd', rounded, value_head_rows)
        return summed / jnp.transpose(totals, (2, 0, 1))[..., None]
    attended = lax.map(attend, query_block_list).reshape(sequence_length, QUERY_HEADS * HEAD_SIZE).astype(jnp.bfloat16)
    mixed_sum = sum_partials(attended, out_weight)
    normed = layer_norm(ALPHA * residual.astype(jnp.float32) + mixed_sum, ln1_gain, ln1_bias).astype(jnp.bfloat16)
    up_acts = jnp.dot(normed, up_weight, preferred_element_type=jnp.float32)
    hidden = jnp.square(jnp.maximum(up_acts, 0.0)).astype(jnp.bfloat16)
    ffn_out = sum_partials(hidden, down_weight)
    return layer_norm(ALPHA * normed.astype(jnp.float32) + ffn_out, ln2_gain, ln2_bias).astype(jnp.bfloat16)
```

```python
import math

import jax
import jax.numpy as jnp
from jax import lax
from jax.experimental import pallas as pl
from jax.experimental.pallas import tpu as pltpu
from jax.sharding import PartitionSpec as P

D = 2048
HEAD_SIZE = 64
GRID_W = 64


ALPHA = 8.0**0.25
ROTARY_BASE = 10000.0
RMS_EPSILON = 1e-06
NORM_EPSILON = 1e-05


def rotate_grid(heads_in, grid_places):
    half_dim = heads_in.shape[-1] // 2
    quarter = half_dim // 2
    inverse = ROTARY_BASE ** (-jnp.arange(quarter, dtype=jnp.float32) / quarter)

    def spin(segment, coords):
        angles = coords.astype(jnp.float32)[:, None] * inverse[None, :]
        cos_val = jnp.cos(angles)[:, None, :]
        sin_val = jnp.sin(angles)[:, None, :]
        lead_half = segment[..., :quarter]
        tail_half = segment[..., quarter:]
        return jnp.concatenate(
            [lead_half * cos_val - tail_half * sin_val, tail_half * cos_val + lead_half * sin_val],
            -1,
        )

    return jnp.concatenate(
        [
            spin(heads_in[..., :half_dim], grid_places // GRID_W),
            spin(heads_in[..., half_dim:], grid_places % GRID_W),
        ],
        -1,
    )


def prepare_inputs(heads_in, gain_vec, grid_places, factor):
    values32 = heads_in.astype(jnp.float32)
    normed = (
        values32
        * lax.rsqrt(jnp.mean(values32 * values32, -1, keepdims=True) + RMS_EPSILON)
        * gain_vec
    )
    return (rotate_grid(normed, grid_places) * factor).astype(jnp.bfloat16)


def layer_norm(pre_norm, gain_vec, bias_vec):
    row_mean = jnp.mean(pre_norm, -1, keepdims=True)
    centred = pre_norm - row_mean
    spread = jnp.mean(centred * centred, -1, keepdims=True)
    return centred * lax.rsqrt(spread + NORM_EPSILON) * gain_vec + bias_vec


def finish_norm(pre_norm, stats, gain_vec, bias_vec):
    row_mean = stats[0][:, None] / D
    spread = stats[1][:, None] / D - row_mean * row_mean
    return (pre_norm - row_mean) * lax.rsqrt(spread + NORM_EPSILON) * gain_vec + bias_vec


def take_cols(array_in, col_start, col_width):
    return lax.dynamic_slice_in_dim(array_in, col_start, col_width, array_in.ndim - 1)


def swap(array_in, axis_name, offset):
    size = lax.axis_size(axis_name)
    return lax.ppermute(array_in, axis_name, [(i, i ^ offset) for i in range(size)])


def gather_low(array_in, low_count, ascending=True):
    bits = [1 << b for b in range(low_count.bit_length() - 1)]
    slots = {0: array_in}
    for bit in bits if ascending else bits[::-1]:
        order = sorted(slots)
        got = swap(jnp.stack([slots[e] for e in order], 0), "sp", bit)
        for n, e in enumerate(order):
            slots[e ^ bit] = got[n]
    return jnp.stack([slots[e] for e in range(low_count)], 0)


def attend_kernel(q_ref, kv_ref, o_ref):
    k = kv_ref[:, :HEAD_SIZE]
    outs = []
    for g in range(q_ref.shape[1] // HEAD_SIZE):
        q = q_ref[:, g * HEAD_SIZE : (g + 1) * HEAD_SIZE]
        scores = lax.dot_general(
            q, k, (((1,), (1,)), ((), ())), preferred_element_type=jnp.float32
        )
        weights = jnp.exp(scores - jnp.max(scores, -1, keepdims=True))
        totals = jnp.sum(weights, -1, keepdims=True)
        summed = jnp.dot(
            weights.astype(jnp.bfloat16), kv_ref[...], preferred_element_type=jnp.float32
        )
        outs.append(summed[:, HEAD_SIZE:] / totals)
    o_ref[...] = jnp.concatenate(outs, 1).astype(jnp.bfloat16)


def attend(q_rows, kv_rows):
    rows, width = q_rows.shape
    keys = kv_rows.shape[0]
    block = math.gcd(rows, max(16, (1 << 20) // keys))
    return pl.pallas_call(
        attend_kernel,
        grid=(rows // block,),
        in_specs=[
            pl.BlockSpec((block, width), lambda i: (i, 0)),
            pl.BlockSpec((keys, kv_rows.shape[1]), lambda i: (0, 0)),
        ],
        out_specs=pl.BlockSpec((block, width), lambda i: (i, 0)),
        out_shape=jax.ShapeDtypeStruct((rows, width), jnp.bfloat16),
    )(q_rows, kv_rows)


def local(
    queries,
    keys,
    values,
    q_gain,
    key_norm_gain,
    out_weight,
    residual,
    ln1_gain,
    ln1_bias,
    up_weight,
    down_weight,
    ln2_gain,
    ln2_bias,
):
    n_sp = lax.axis_size("sp")
    n_tp = lax.axis_size("tp")
    split = math.gcd(n_sp, 4)
    low_count = n_sp // split
    me = lax.axis_index("sp")
    hi = me // low_count
    core = lax.axis_index("tp")

    tok_rows = queries.shape[0]
    grid_places = me * tok_rows + jnp.arange(tok_rows, dtype=jnp.int32)
    kv_heads = keys.shape[1] // HEAD_SIZE
    q_count = queries.shape[1] // HEAD_SIZE
    group = q_count // kv_heads
    q_sent = prepare_inputs(
        queries.reshape(tok_rows, q_count, HEAD_SIZE), q_gain, grid_places, HEAD_SIZE ** (-0.5)
    ).reshape(tok_rows, kv_heads, group * HEAD_SIZE)
    k_sent = prepare_inputs(
        keys.reshape(tok_rows, kv_heads, HEAD_SIZE), key_norm_gain, grid_places, 1.0
    )
    v_sent = values.reshape(tok_rows, kv_heads, HEAD_SIZE)
    packed = jnp.concatenate([q_sent, k_sent, v_sent], -1)
    packed = jnp.transpose(packed, (1, 0, 2))
    q_width = group * HEAD_SIZE

    if kv_heads % split == 0:
        per = kv_heads // split
        parts = []
        for d in range(split):
            block = lax.dynamic_slice_in_dim(packed, (hi ^ d) * per, per, 0)
            parts.append(block if d == 0 else swap(block, "sp", d * low_count))
        got = jnp.concatenate(parts, 1)
        kv_all = gather_low(got[..., q_width:], low_count)
        heads_out = []
        for h in range(per):
            kv_rows = kv_all[:, h].reshape(-1, 2 * HEAD_SIZE)
            heads_out.append(attend(got[h, :, :q_width], kv_rows))
        att = jnp.concatenate(heads_out, 1)
        width = att.shape[1]
        attended = jnp.zeros((tok_rows, split * width), jnp.bfloat16)
        for d in range(split):
            block = att[d * tok_rows : (d + 1) * tok_rows]
            if d:
                block = swap(block, "sp", d * low_count)
            attended = lax.dynamic_update_slice_in_dim(attended, block, (hi ^ d) * width, 1)
    else:
        kv_all = lax.all_gather(packed[..., q_width:], "sp", axis=1, tiled=True)
        attended = jnp.concatenate(
            [attend(packed[h, :, :q_width], kv_all[h]) for h in range(kv_heads)], 1
        )

    ff_own = up_weight.shape[1] // split
    up_parts, down_parts = [], []
    for d in range(split):
        start = (hi ^ d) * ff_own
        up_block = lax.dynamic_slice_in_dim(up_weight, start, ff_own, 1)
        down_block = lax.dynamic_slice_in_dim(down_weight, start, ff_own, 0)
        if d:
            up_block = swap(up_block, "sp", d * low_count)
            down_block = swap(down_block, "sp", d * low_count)
        up_parts.append(up_block)
        down_parts.append(down_block)
    up_all = gather_low(jnp.stack(up_parts, 0), low_count)
    down_all = gather_low(jnp.stack(down_parts, 0), low_count, ascending=False)

    def placed(pieces, axis):
        ordered = []
        for s in range(n_sp):
            rel = me ^ s
            piece = lax.dynamic_slice(
                pieces,
                (rel % low_count, rel // low_count, 0, 0),
                (1, 1) + pieces.shape[2:],
            )
            ordered.append(piece.reshape(pieces.shape[2:]))
        return jnp.concatenate(ordered, axis)

    up_own = placed(up_all, 0)
    down_own = placed(down_all, 1)

    mixed_sum = jnp.zeros((tok_rows, D), jnp.float32)
    for d in range(n_tp):
        att_d = attended if d == 0 else swap(attended, "tp", d)
        w_d = out_weight if d == 0 else swap(out_weight, "tp", d)
        partial_value = jnp.dot(att_d, w_d, preferred_element_type=jnp.float32)
        mixed_sum = mixed_sum + partial_value.astype(jnp.bfloat16).astype(jnp.float32)
    full_rows = layer_norm(
        ALPHA * residual.astype(jnp.float32) + mixed_sum, ln1_gain, ln1_bias
    ).astype(jnp.bfloat16)

    col_width = D // n_tp
    normed_own = take_cols(full_rows, core * col_width, col_width)

    ffn_cols = jnp.zeros((tok_rows, col_width), jnp.float32)
    for d in range(split):
        if d == 0:
            rows_d = full_rows
        else:
            mine = swap(normed_own, "sp", d * low_count)
            rows_d = jnp.zeros((tok_rows, D), jnp.bfloat16)
            for e in range(n_tp):
                piece = mine if e == 0 else swap(mine, "tp", e)
                rows_d = lax.dynamic_update_slice_in_dim(
                    rows_d, piece, (core ^ e) * col_width, 1
                )
        up_acts = jnp.dot(rows_d, up_own, preferred_element_type=jnp.float32)
        hidden = jnp.square(jnp.maximum(up_acts, 0.0)).astype(jnp.bfloat16)
        partial_ffn = jnp.dot(hidden, down_own, preferred_element_type=jnp.float32).astype(
            jnp.bfloat16
        )
        cols = jnp.zeros((tok_rows, col_width), jnp.float32)
        for e in range(n_tp):
            piece = take_cols(partial_ffn, (core ^ e) * col_width, col_width)
            if e:
                piece = swap(piece, "tp", e)
            cols = cols + piece.astype(jnp.float32)
        if d:
            cols = swap(cols.astype(jnp.bfloat16), "sp", d * low_count).astype(jnp.float32)
        ffn_cols = ffn_cols + cols

    second = ALPHA * normed_own.astype(jnp.float32) + ffn_cols
    stats_two = lax.psum((jnp.sum(second, -1), jnp.sum(second * second, -1)), "tp")
    return finish_norm(
        second,
        stats_two,
        take_cols(ln2_gain, core * col_width, col_width),
        take_cols(ln2_bias, core * col_width, col_width),
    ).astype(jnp.bfloat16)


def solution(mesh):
    return jax.shard_map(
        local,
        mesh=mesh,
        in_specs=(
            P("sp", "tp"),
            P("sp", "tp"),
            P("sp", "tp"),
            P(),
            P(),
            P("tp", None),
            P("sp", None),
            P(),
            P(),
            P("sp", "tp"),
            P("tp", "sp"),
            P(),
            P(),
        ),
        out_specs=P("sp", "tp"),
        check_vma=False,
    )
```

```python
import math

import jax
import jax.numpy as jnp
from jax import lax
from jax.experimental import pallas as pl
from jax.experimental.pallas import tpu as pltpu
from jax.sharding import PartitionSpec as P

D = 2048
HEAD_SIZE = 64
GRID_W = 64


ALPHA = 8.0**0.25
ROTARY_BASE = 10000.0
RMS_EPSILON = 1e-06
NORM_EPSILON = 1e-05


def rotate_grid(heads_in, grid_places):
    half_dim = heads_in.shape[-1] // 2
    quarter = half_dim // 2
    inverse = ROTARY_BASE ** (-jnp.arange(quarter, dtype=jnp.float32) / quarter)

    def spin(segment, coords):
        angles = coords.astype(jnp.float32)[:, None] * inverse[None, :]
        cos_val = jnp.cos(angles)[:, None, :]
        sin_val = jnp.sin(angles)[:, None, :]
        lead_half = segment[..., :quarter]
        tail_half = segment[..., quarter:]
        return jnp.concatenate(
            [lead_half * cos_val - tail_half * sin_val, tail_half * cos_val + lead_half * sin_val],
            -1,
        )

    return jnp.concatenate(
        [
            spin(heads_in[..., :half_dim], grid_places // GRID_W),
            spin(heads_in[..., half_dim:], grid_places % GRID_W),
        ],
        -1,
    )


def prepare_inputs(heads_in, gain_vec, grid_places, factor):
    values32 = heads_in.astype(jnp.float32)
    normed = (
        values32
        * lax.rsqrt(jnp.mean(values32 * values32, -1, keepdims=True) + RMS_EPSILON)
        * gain_vec
    )
    return (rotate_grid(normed, grid_places) * factor).astype(jnp.bfloat16)


def layer_norm(pre_norm, gain_vec, bias_vec):
    row_mean = jnp.mean(pre_norm, -1, keepdims=True)
    centred = pre_norm - row_mean
    spread = jnp.mean(centred * centred, -1, keepdims=True)
    return centred * lax.rsqrt(spread + NORM_EPSILON) * gain_vec + bias_vec


def finish_norm(pre_norm, stats, gain_vec, bias_vec):
    row_mean = stats[0][:, None] / D
    spread = stats[1][:, None] / D - row_mean * row_mean
    return (pre_norm - row_mean) * lax.rsqrt(spread + NORM_EPSILON) * gain_vec + bias_vec


def take_cols(array_in, col_start, col_width):
    return lax.dynamic_slice_in_dim(array_in, col_start, col_width, array_in.ndim - 1)


def swap(array_in, axis_name, offset):
    size = lax.axis_size(axis_name)
    return lax.ppermute(array_in, axis_name, [(i, i ^ offset) for i in range(size)])


def gather_low(array_in, low_count, ascending=True):
    bits = [1 << b for b in range(low_count.bit_length() - 1)]
    slots = {0: array_in}
    for bit in bits if ascending else bits[::-1]:
        for e in sorted(slots):
            slots[e ^ bit] = swap(slots[e], "sp", bit)
    return [slots[e] for e in range(low_count)]


def place_blocks(pieces, me, core, n_tp, axis):
    low_count = len(pieces)
    split, rows, cols = pieces[0].shape
    n_sp = low_count * split
    width = (rows, cols)[axis]
    part = n_sp * width // n_tp
    out_shape = (n_sp * rows, cols) if axis == 0 else (rows, n_sp * cols)
    starts = []
    for e in range(low_count):
        for d in range(split):
            at = (me ^ (d * low_count + e)) * width
            starts.append(((at // part) ^ core) * part + at % part)

    if width % 128:
        out = jnp.zeros(out_shape, jnp.bfloat16)
        for n, at in enumerate(starts):
            out = lax.dynamic_update_slice_in_dim(out, pieces[n // split][n % split], at, axis)
        return out

    def kernel(starts_ref, *refs):
        o_ref = refs[-1]
        for e in range(low_count):
            for d in range(split):
                at = pl.multiple_of(starts_ref[e * split + d], 128)
                if axis == 0:
                    o_ref[pl.ds(at, rows), :] = refs[e][d]
                else:
                    o_ref[:, pl.ds(at, cols)] = refs[e][d]

    return pl.pallas_call(
        kernel,
        in_specs=[pl.BlockSpec(memory_space=pltpu.SMEM)]
        + [pl.BlockSpec(memory_space=pltpu.VMEM)] * low_count,
        out_specs=pl.BlockSpec(memory_space=pltpu.VMEM),
        out_shape=jax.ShapeDtypeStruct(out_shape, jnp.bfloat16),
    )(jnp.stack(starts).astype(jnp.int32), *pieces)


def attend_kernel(q_ref, kv_ref, o_ref):
    k = kv_ref[:, :HEAD_SIZE]
    outs = []
    for g in range(q_ref.shape[1] // HEAD_SIZE):
        q = q_ref[:, g * HEAD_SIZE : (g + 1) * HEAD_SIZE]
        scores = lax.dot_general(
            q, k, (((1,), (1,)), ((), ())), preferred_element_type=jnp.float32
        )
        weights = jnp.exp(scores - jnp.max(scores, -1, keepdims=True))
        totals = jnp.sum(weights, -1, keepdims=True)
        summed = jnp.dot(
            weights.astype(jnp.bfloat16), kv_ref[...], preferred_element_type=jnp.float32
        )
        outs.append(summed[:, HEAD_SIZE:] / totals)
    o_ref[...] = jnp.concatenate(outs, 1).astype(jnp.bfloat16)


def attend(q_rows, kv_rows):
    rows, width = q_rows.shape
    keys = kv_rows.shape[0]
    block = math.gcd(rows, max(16, (1 << 20) // keys))
    return pl.pallas_call(
        attend_kernel,
        grid=(rows // block,),
        in_specs=[
            pl.BlockSpec((block, width), lambda i: (i, 0)),
            pl.BlockSpec((keys, kv_rows.shape[1]), lambda i: (0, 0)),
        ],
        out_specs=pl.BlockSpec((block, width), lambda i: (i, 0)),
        out_shape=jax.ShapeDtypeStruct((rows, width), jnp.bfloat16),
    )(q_rows, kv_rows)


def local(
    queries,
    keys,
    values,
    q_gain,
    key_norm_gain,
    out_weight,
    residual,
    ln1_gain,
    ln1_bias,
    up_weight,
    down_weight,
    ln2_gain,
    ln2_bias,
):
    n_sp = lax.axis_size("sp")
    n_tp = lax.axis_size("tp")
    split = math.gcd(n_sp, 4)
    low_count = n_sp // split
    me = lax.axis_index("sp")
    hi = me // low_count
    core = lax.axis_index("tp")

    tok_rows = queries.shape[0]
    grid_places = me * tok_rows + jnp.arange(tok_rows, dtype=jnp.int32)
    kv_heads = keys.shape[1] // HEAD_SIZE
    q_count = queries.shape[1] // HEAD_SIZE
    group = q_count // kv_heads
    q_sent = prepare_inputs(
        queries.reshape(tok_rows, q_count, HEAD_SIZE), q_gain, grid_places, HEAD_SIZE ** (-0.5)
    ).reshape(tok_rows, kv_heads, group * HEAD_SIZE)
    k_sent = prepare_inputs(
        keys.reshape(tok_rows, kv_heads, HEAD_SIZE), key_norm_gain, grid_places, 1.0
    )
    v_sent = values.reshape(tok_rows, kv_heads, HEAD_SIZE)
    packed = jnp.concatenate([q_sent, k_sent, v_sent], -1)
    packed = jnp.transpose(packed, (1, 0, 2))
    q_width = group * HEAD_SIZE

    if kv_heads % split == 0:
        per = kv_heads // split
        parts = []
        for d in range(split):
            block = lax.dynamic_slice_in_dim(packed, (hi ^ d) * per, per, 0)
            parts.append(block if d == 0 else swap(block, "sp", d * low_count))
        got = jnp.concatenate(parts, 1)
        kv_all = jnp.stack(gather_low(got[..., q_width:], low_count), 0)
        heads_out = []
        for h in range(per):
            kv_rows = kv_all[:, h].reshape(-1, 2 * HEAD_SIZE)
            heads_out.append(attend(got[h, :, :q_width], kv_rows))
        att = jnp.concatenate(heads_out, 1)
        width = att.shape[1]
        attended = jnp.zeros((tok_rows, split * width), jnp.bfloat16)
        for d in range(split):
            block = att[d * tok_rows : (d + 1) * tok_rows]
            if d:
                block = swap(block, "sp", d * low_count)
            attended = lax.dynamic_update_slice_in_dim(attended, block, (hi ^ d) * width, 1)
    else:
        kv_all = lax.all_gather(packed[..., q_width:], "sp", axis=1, tiled=True)
        attended = jnp.concatenate(
            [attend(packed[h, :, :q_width], kv_all[h]) for h in range(kv_heads)], 1
        )

    ff_own = up_weight.shape[1] // split
    up_parts, down_parts = [], []
    for d in range(split):
        start = (hi ^ d) * ff_own
        up_block = lax.dynamic_slice_in_dim(up_weight, start, ff_own, 1)
        down_block = lax.dynamic_slice_in_dim(down_weight, start, ff_own, 0)
        if d:
            up_block = swap(up_block, "sp", d * low_count)
            down_block = swap(down_block, "sp", d * low_count)
        up_parts.append(up_block)
        down_parts.append(down_block)
    up_all = gather_low(jnp.stack(up_parts, 0), low_count)
    down_all = gather_low(jnp.stack(down_parts, 0), low_count, ascending=False)
    up_own = place_blocks(up_all, me, core, n_tp, 0)
    down_own = place_blocks(down_all, me, core, n_tp, 1)

    mixed_sum = jnp.zeros((tok_rows, D), jnp.float32)
    for d in range(n_tp):
        att_d = attended if d == 0 else swap(attended, "tp", d)
        w_d = out_weight if d == 0 else swap(out_weight, "tp", d)
        partial_value = jnp.dot(att_d, w_d, preferred_element_type=jnp.float32)
        mixed_sum = mixed_sum + partial_value.astype(jnp.bfloat16).astype(jnp.float32)
    full_rows = layer_norm(
        ALPHA * residual.astype(jnp.float32) + mixed_sum, ln1_gain, ln1_bias
    ).astype(jnp.bfloat16)

    col_width = D // n_tp
    normed_own = take_cols(full_rows, core * col_width, col_width)

    ffn_cols = jnp.zeros((tok_rows, col_width), jnp.float32)
    for d in [*range(1, split), 0]:
        if d == 0:
            pieces = [
                take_cols(full_rows, (core ^ e) * col_width, col_width) for e in range(n_tp)
            ]
        else:
            mine = swap(normed_own, "sp", d * low_count)
            pieces = [mine] + [swap(mine, "tp", e) for e in range(1, n_tp)]
        rows_d = jnp.concatenate(pieces, 1)
        up_acts = jnp.dot(rows_d, up_own, preferred_element_type=jnp.float32)
        hidden = jnp.square(jnp.maximum(up_acts, 0.0)).astype(jnp.bfloat16)
        partial_ffn = jnp.dot(hidden, down_own, preferred_element_type=jnp.float32).astype(
            jnp.bfloat16
        )
        cols = jnp.zeros((tok_rows, col_width), jnp.float32)
        for e in range(n_tp):
            piece = partial_ffn[:, e * col_width : (e + 1) * col_width]
            if e:
                piece = swap(piece, "tp", e)
            cols = cols + piece.astype(jnp.float32)
        if d:
            cols = swap(cols.astype(jnp.bfloat16), "sp", d * low_count).astype(jnp.float32)
        ffn_cols = ffn_cols + cols

    second = ALPHA * normed_own.astype(jnp.float32) + ffn_cols
    stats_two = lax.psum((jnp.sum(second, -1), jnp.sum(second * second, -1)), "tp")
    return finish_norm(
        second,
        stats_two,
        take_cols(ln2_gain, core * col_width, col_width),
        take_cols(ln2_bias, core * col_width, col_width),
    ).astype(jnp.bfloat16)


def solution(mesh):
    return jax.shard_map(
        local,
        mesh=mesh,
        in_specs=(
            P("sp", "tp"),
            P("sp", "tp"),
            P("sp", "tp"),
            P(),
            P(),
            P("tp", None),
            P("sp", None),
            P(),
            P(),
            P("sp", "tp"),
            P("tp", "sp"),
            P(),
            P(),
        ),
        out_specs=P("sp", "tp"),
        check_vma=False,
    )
```

```python
import math

import jax
import jax.numpy as jnp
from jax import lax
from jax.experimental import pallas as pl
from jax.experimental.pallas import tpu as pltpu
from jax.sharding import PartitionSpec as P

D = 2048
HEAD_SIZE = 64
GRID_W = 64


ALPHA = 8.0**0.25
ROTARY_BASE = 10000.0
RMS_EPSILON = 1e-06
NORM_EPSILON = 1e-05


def rotate_grid(heads_in, grid_places):
    half_dim = heads_in.shape[-1] // 2
    quarter = half_dim // 2
    inverse = ROTARY_BASE ** (-jnp.arange(quarter, dtype=jnp.float32) / quarter)

    def spin(segment, coords):
        angles = coords.astype(jnp.float32)[:, None] * inverse[None, :]
        cos_val = jnp.cos(angles)[:, None, :]
        sin_val = jnp.sin(angles)[:, None, :]
        lead_half = segment[..., :quarter]
        tail_half = segment[..., quarter:]
        return jnp.concatenate(
            [lead_half * cos_val - tail_half * sin_val, tail_half * cos_val + lead_half * sin_val],
            -1,
        )

    return jnp.concatenate(
        [
            spin(heads_in[..., :half_dim], grid_places // GRID_W),
            spin(heads_in[..., half_dim:], grid_places % GRID_W),
        ],
        -1,
    )


def prepare_inputs(heads_in, gain_vec, grid_places, factor):
    values32 = heads_in.astype(jnp.float32)
    normed = (
        values32
        * lax.rsqrt(jnp.mean(values32 * values32, -1, keepdims=True) + RMS_EPSILON)
        * gain_vec
    )
    return (rotate_grid(normed, grid_places) * factor).astype(jnp.bfloat16)


def layer_norm(pre_norm, gain_vec, bias_vec):
    row_mean = jnp.mean(pre_norm, -1, keepdims=True)
    centred = pre_norm - row_mean
    spread = jnp.mean(centred * centred, -1, keepdims=True)
    return centred * lax.rsqrt(spread + NORM_EPSILON) * gain_vec + bias_vec


def finish_norm(pre_norm, stats, gain_vec, bias_vec):
    row_mean = stats[0][:, None] / D
    spread = stats[1][:, None] / D - row_mean * row_mean
    return (pre_norm - row_mean) * lax.rsqrt(spread + NORM_EPSILON) * gain_vec + bias_vec


def take_cols(array_in, col_start, col_width):
    return lax.dynamic_slice_in_dim(array_in, col_start, col_width, array_in.ndim - 1)


def swap(array_in, axis_name, offset):
    size = lax.axis_size(axis_name)
    return lax.ppermute(array_in, axis_name, [(i, i ^ offset) for i in range(size)])


def gather_low(array_in, low_count, ascending=True):
    bits = [1 << b for b in range(low_count.bit_length() - 1)]
    slots = {0: array_in}
    for bit in bits if ascending else bits[::-1]:
        for e in sorted(slots):
            slots[e ^ bit] = swap(slots[e], "sp", bit)
    return [slots[e] for e in range(low_count)]


def place_blocks(pieces, me, core, n_tp, axis):
    low_count = len(pieces)
    split, rows, cols = pieces[0].shape
    n_sp = low_count * split
    width = (rows, cols)[axis]
    part = n_sp * width // n_tp
    out_shape = (n_sp * rows, cols) if axis == 0 else (rows, n_sp * cols)
    starts = []
    for e in range(low_count):
        for d in range(split):
            at = (me ^ (d * low_count + e)) * width
            starts.append(((at // part) ^ core) * part + at % part)

    if width % 128:
        out = jnp.zeros(out_shape, jnp.bfloat16)
        for n, at in enumerate(starts):
            out = lax.dynamic_update_slice_in_dim(out, pieces[n // split][n % split], at, axis)
        return out

    def kernel(starts_ref, *refs):
        o_ref = refs[-1]
        for e in range(low_count):
            for d in range(split):
                at = pl.multiple_of(starts_ref[e * split + d], 128)
                if axis == 0:
                    o_ref[pl.ds(at, rows), :] = refs[e][d]
                else:
                    o_ref[:, pl.ds(at, cols)] = refs[e][d]

    return pl.pallas_call(
        kernel,
        in_specs=[pl.BlockSpec(memory_space=pltpu.SMEM)]
        + [pl.BlockSpec(memory_space=pltpu.VMEM)] * low_count,
        out_specs=pl.BlockSpec(memory_space=pltpu.VMEM),
        out_shape=jax.ShapeDtypeStruct(out_shape, jnp.bfloat16),
    )(jnp.stack(starts).astype(jnp.int32), *pieces)


def attend_kernel(q_ref, kv_ref, o_ref):
    k = kv_ref[:, :HEAD_SIZE]
    outs = []
    for g in range(q_ref.shape[1] // HEAD_SIZE):
        q = q_ref[:, g * HEAD_SIZE : (g + 1) * HEAD_SIZE]
        scores = lax.dot_general(
            q, k, (((1,), (1,)), ((), ())), preferred_element_type=jnp.float32
        )
        weights = jnp.exp(scores - jnp.max(scores, -1, keepdims=True))
        totals = jnp.sum(weights, -1, keepdims=True)
        summed = jnp.dot(
            weights.astype(jnp.bfloat16), kv_ref[...], preferred_element_type=jnp.float32
        )
        outs.append(summed[:, HEAD_SIZE:] / totals)
    o_ref[...] = jnp.concatenate(outs, 1).astype(jnp.bfloat16)


def attend(q_rows, kv_rows):
    rows, width = q_rows.shape
    keys = kv_rows.shape[0]
    block = math.gcd(rows, max(16, (1 << 20) // keys))
    return pl.pallas_call(
        attend_kernel,
        grid=(rows // block,),
        in_specs=[
            pl.BlockSpec((block, width), lambda i: (i, 0)),
            pl.BlockSpec((keys, kv_rows.shape[1]), lambda i: (0, 0)),
        ],
        out_specs=pl.BlockSpec((block, width), lambda i: (i, 0)),
        out_shape=jax.ShapeDtypeStruct((rows, width), jnp.bfloat16),
    )(q_rows, kv_rows)


def local(
    queries,
    keys,
    values,
    q_gain,
    key_norm_gain,
    out_weight,
    residual,
    ln1_gain,
    ln1_bias,
    up_weight,
    down_weight,
    ln2_gain,
    ln2_bias,
):
    n_sp = lax.axis_size("sp")
    n_tp = lax.axis_size("tp")
    split = math.gcd(n_sp, 4)
    low_count = n_sp // split
    me = lax.axis_index("sp")
    hi = me // low_count
    core = lax.axis_index("tp")

    tok_rows = queries.shape[0]
    grid_places = me * tok_rows + jnp.arange(tok_rows, dtype=jnp.int32)
    kv_heads = keys.shape[1] // HEAD_SIZE
    q_count = queries.shape[1] // HEAD_SIZE
    group = q_count // kv_heads
    q_sent = prepare_inputs(
        queries.reshape(tok_rows, q_count, HEAD_SIZE), q_gain, grid_places, HEAD_SIZE ** (-0.5)
    ).reshape(tok_rows, kv_heads, group * HEAD_SIZE)
    k_sent = prepare_inputs(
        keys.reshape(tok_rows, kv_heads, HEAD_SIZE), key_norm_gain, grid_places, 1.0
    )
    v_sent = values.reshape(tok_rows, kv_heads, HEAD_SIZE)
    packed = jnp.concatenate([q_sent, k_sent, v_sent], -1)
    packed = jnp.transpose(packed, (1, 0, 2))
    q_width = group * HEAD_SIZE

    if kv_heads % split == 0:
        per = kv_heads // split
        parts = []
        for d in range(split):
            block = lax.dynamic_slice_in_dim(packed, (hi ^ d) * per, per, 0)
            parts.append(block if d == 0 else swap(block, "sp", d * low_count))
        got = jnp.concatenate(parts, 1)
        kv_all = jnp.stack(gather_low(got[..., q_width:], low_count), 0)
        heads_out = []
        for h in range(per):
            kv_rows = kv_all[:, h].reshape(-1, 2 * HEAD_SIZE)
            heads_out.append(attend(got[h, :, :q_width], kv_rows))
        att = jnp.concatenate(heads_out, 1)
        width = att.shape[1]
        attended = jnp.zeros((tok_rows, split * width), jnp.bfloat16)
        for d in range(split):
            block = att[d * tok_rows : (d + 1) * tok_rows]
            if d:
                block = swap(block, "sp", d * low_count)
            attended = lax.dynamic_update_slice_in_dim(attended, block, (hi ^ d) * width, 1)
    else:
        kv_all = lax.all_gather(packed[..., q_width:], "sp", axis=1, tiled=True)
        attended = jnp.concatenate(
            [attend(packed[h, :, :q_width], kv_all[h]) for h in range(kv_heads)], 1
        )

    ff_own = up_weight.shape[1] // split
    up_parts, down_parts = [], []
    for d in range(split):
        start = (hi ^ d) * ff_own
        up_block = lax.dynamic_slice_in_dim(up_weight, start, ff_own, 1)
        down_block = lax.dynamic_slice_in_dim(down_weight, start, ff_own, 0)
        if d:
            up_block = swap(up_block, "sp", d * low_count)
            down_block = swap(down_block, "sp", d * low_count)
        up_parts.append(up_block)
        down_parts.append(down_block)
    up_all = gather_low(jnp.stack(up_parts, 0), low_count)
    down_all = gather_low(jnp.stack(down_parts, 0), low_count, ascending=False)
    up_own = place_blocks(up_all, me, core, n_tp, 0)
    down_own = place_blocks(down_all, me, core, n_tp, 1)

    mixed_sum = jnp.zeros((tok_rows, D), jnp.float32)
    for d in range(n_tp):
        att_d = attended if d == 0 else swap(attended, "tp", d)
        w_d = out_weight if d == 0 else swap(out_weight, "tp", d)
        partial_value = jnp.dot(att_d, w_d, preferred_element_type=jnp.float32)
        mixed_sum = mixed_sum + partial_value.astype(jnp.bfloat16).astype(jnp.float32)
    full_rows = layer_norm(
        ALPHA * residual.astype(jnp.float32) + mixed_sum, ln1_gain, ln1_bias
    ).astype(jnp.bfloat16)

    col_width = D // n_tp
    normed_own = take_cols(full_rows, core * col_width, col_width)

    ffn_cols = jnp.zeros((tok_rows, col_width), jnp.float32)
    for d in [*range(2, split), 1, 0][-split:]:
        if d == 0:
            pieces = [
                take_cols(full_rows, (core ^ e) * col_width, col_width) for e in range(n_tp)
            ]
        else:
            mine = swap(normed_own, "sp", d * low_count)
            pieces = [mine] + [swap(mine, "tp", e) for e in range(1, n_tp)]
        rows_d = jnp.concatenate(pieces, 1)
        up_acts = jnp.dot(rows_d, up_own, preferred_element_type=jnp.float32)
        hidden = jnp.square(jnp.maximum(up_acts, 0.0)).astype(jnp.bfloat16)
        partial_ffn = jnp.dot(hidden, down_own, preferred_element_type=jnp.float32).astype(
            jnp.bfloat16
        )
        cols = jnp.zeros((tok_rows, col_width), jnp.float32)
        for e in range(n_tp):
            piece = partial_ffn[:, e * col_width : (e + 1) * col_width]
            if e:
                piece = swap(piece, "tp", e)
            cols = cols + piece.astype(jnp.float32)
        if d:
            cols = swap(cols.astype(jnp.bfloat16), "sp", d * low_count)
            cols = cols.astype(jnp.float32)
        ffn_cols = ffn_cols + cols

    second = ALPHA * normed_own.astype(jnp.float32) + ffn_cols
    stats_two = lax.psum((jnp.sum(second, -1), jnp.sum(second * second, -1)), "tp")
    return finish_norm(
        second,
        stats_two,
        take_cols(ln2_gain, core * col_width, col_width),
        take_cols(ln2_bias, core * col_width, col_width),
    ).astype(jnp.bfloat16)


def solution(mesh):
    return jax.shard_map(
        local,
        mesh=mesh,
        in_specs=(
            P("sp", "tp"),
            P("sp", "tp"),
            P("sp", "tp"),
            P(),
            P(),
            P("tp", None),
            P("sp", None),
            P(),
            P(),
            P("sp", "tp"),
            P("tp", "sp"),
            P(),
            P(),
        ),
        out_specs=P("sp", "tp"),
        check_vma=False,
    )
```
